256 devices in a mesh: grp: 2 (over y), fs: 32 (over z, core), tp: 4 (over x).
Axes of the slice: x: 4, y: 2, z: 16, core: 2. Of those that a mesh axis runs over, the one named last changes fastest.
The devices are a block of a 4x16x16 slice.
Arguments:
- tokens: bfloat16 [24576, 4096], P(('grp', 'fs'), 'tp'), parts along dimension 0, may hold values from -1100 to 1100
- norm_gain: float32 [4096], P('fs'), may hold values from 0.1 to 1.9
- gate_master: float32 [32, 4096, 512], P(None, 'fs', 'tp'), may hold values from -0.09375 to 0.09375
- up_master: float32 [32, 4096, 512], P(None, 'fs', 'tp'), may hold values from -0.09375 to 0.09375
- down_master: float32 [32, 512, 4096], P(None, 'fs', 'tp'), may hold values from -0.25 to 0.25
- expert_ids: int32 [24576, 2], P(('grp', 'fs')), parts along dimension 0, may hold values from 0 to 31, as said below
- route_weights: float32 [24576, 2], P(('grp', 'fs')), parts along dimension 0, may hold values from 0.2 to 1
Outputs:
- gate_sampler: bfloat16 [64, 4096, 512], P(('grp', 'fs'), None, 'tp'), parts along dimension 0
- up_sampler: bfloat16 [64, 4096, 512], P(('grp', 'fs'), None, 'tp'), parts along dimension 0
- down_sampler: bfloat16 [64, 512, 4096], P(('grp', 'fs'), 'tp'), parts along dimension 0
- mixed: bfloat16 [24576, 4096], P(('grp', 'fs'), 'tp'), parts along dimension 0
The draws below stay inside these ranges and needn't reach their ends.
There are 2 independent parts, one for each index of `grp`. The reference program is written for one: setup_inputs(seed, part) draws one part's arguments, and reference() takes and returns one part's arrays. A program takes and returns all parts, laid end to end along the dimension named above; an argument that names none is the same for every part. Nothing has to cross between parts.
Inputs may be any that keep to these rules, and one draw needn't show every extreme that they name: `expert_ids`: each row names two different experts of one group: experts g * 8 to (g + 1) * 8 - 1 for some g. In each aligned block of 384 rows every expert is named exactly 24 times.
All inputs are finite; a program needn't handle non-finite values.
Results may differ from the reference program's by a relative error of at most 0.0091.
Values may be sent and summed in bfloat16 or wider, within the bound.
No kernel may reach another device: no remote copies, remote signals or barrier semaphores. Data moves between devices by JAX's collectives and lax.ppermute only.
A program may use at most 128 MiB of HBM per device.

```python
import math
import jax
import jax.numpy as jnp
from jax import lax

D = 4096
FF = 512
TOP = 2
TOK_DEV = 384
EXPERTS = 32
GROUPS = 4
TOKENS = 12288
N_TP = 4


def draw_tokens(key, part):
    k_base, k_column, k_row = jax.random.split(jax.random.fold_in(key, 3), 3)
    column = jnp.arange(D, dtype=jnp.float32) / D
    column_scale = 10.0 ** column * jnp.exp(jax.random.uniform(k_column, (D,), jnp.float32, -0.7, 0.7))
    row_scale = jnp.exp(jax.random.uniform(k_row, (TOKENS, 1), jnp.float32, 0.0, math.log(10.0)))
    base = jax.random.normal(k_base, (TOKENS, D), jnp.float32)
    base = jnp.clip(base, -5.0, 5.0)
    return (base * column_scale[None, :] * row_scale).astype(jnp.bfloat16)


def draw_expert_ids(key, part):
    blocks = TOKENS // TOK_DEV
    per_group = EXPERTS // GROUPS
    keys = jax.random.split(jax.random.fold_in(key, 11), blocks)

    def one_block(block_key):
        k_rank, k_turn = jax.random.split(block_key)
        rank = jax.random.permutation(k_rank, TOK_DEV).astype(jnp.int32)
        group = rank % GROUPS
        within = rank // GROUPS
        turn = jax.random.randint(k_turn, (GROUPS,), 0, per_group).astype(jnp.int32)
        first = (within + turn[group]) % per_group
        stride = 1 + within // per_group % (per_group - 1)
        second = (first + stride) % per_group
        return jnp.stack([group * per_group + first, group * per_group + second], axis=1)
    return jax.vmap(one_block)(keys).reshape(TOKENS, TOP).astype(jnp.int32)


def block_levels(key, shape, cuts, low, top_value):
    def one(axis_at, blocks):
        heights = jax.random.uniform(jax.random.fold_in(jax.random.fold_in(key, 6), axis_at), (blocks,), jnp.float32, low / len(cuts), top_value / len(cuts))
        return jnp.repeat(jnp.exp(heights), shape[axis_at] // blocks).reshape((-1,) + (1,) * (len(shape) - axis_at - 1))

    level = one(*cuts[0])
    for cut in cuts[1:]:
        level = level * one(*cut)
    return level


def bell_draw(own_key, shape, width, reach, cuts=(), kind=jnp.bfloat16):
    result = width * jax.random.normal(own_key, shape, jnp.float32)
    if cuts:
        result = result * block_levels(own_key, shape, cuts, -0.22, 0.18)
    return jnp.clip(result, -reach, reach).astype(kind)


def setup_inputs(seed: int = 0, part: int = 0) -> dict:
    seeds = jax.random.split(jax.random.key(seed), 8)
    part_splits = jax.random.split(jax.random.fold_in(seeds[7], part), 8)
    return {
        "tokens": draw_tokens(jax.random.fold_in(jax.random.fold_in(seeds[7], part), 71), part),
        "norm_gain": jnp.clip(1.0 + 0.18 * jax.random.normal(seeds[1], (D,), jnp.float32), 0.1, 1.9),
        "gate_master": bell_draw(seeds[2], (EXPERTS, D, FF), D ** -0.5, 0.09375, ((1, 32), (2, 4)), jnp.float32),
        "up_master": bell_draw(seeds[3], (EXPERTS, D, FF), D ** -0.5, 0.09375, ((1, 32), (2, 4)), jnp.float32),
        "down_master": bell_draw(seeds[4], (EXPERTS, FF, D), FF ** -0.5, 0.25, ((1, 32), (2, 4)), jnp.float32),
        "expert_ids": draw_expert_ids(jax.random.fold_in(jax.random.fold_in(seeds[7], part), 71), part),
        "route_weights": jnp.clip(jnp.exp(math.log(1.0) - 1.609438 * jax.random.uniform(part_splits[6], (TOKENS, TOP), jnp.float32) ** block_levels(part_splits[6], (TOKENS, TOP), ((0, 32),), -0.2, 0.2)), 0.2, 1.0),
    }


def reference(tokens, norm_gain, gate_master, up_master, down_master, expert_ids, route_weights):
    gate_w = (norm_gain[None, :, None] * gate_master).astype(jnp.bfloat16)
    up_w = (norm_gain[None, :, None] * up_master).astype(jnp.bfloat16)
    down_w = down_master.astype(jnp.bfloat16)
    values = tokens.astype(jnp.float32)
    normed = (values * lax.rsqrt(lax.optimization_barrier(jnp.mean(values * values, axis=1, keepdims=True)) + 1e-06)).astype(jnp.bfloat16)
    flat = expert_ids.reshape(-1)
    order = jnp.argsort(flat, stable=True).astype(jnp.int32)
    per_expert = flat.shape[0] // EXPERTS
    owners = (order // TOP).astype(jnp.int32).reshape(EXPERTS, per_expert)
    weights = route_weights.reshape(-1)[order].reshape(EXPERTS, per_expert)
    block = FF // N_TP

    def run_expert(inputs):
        e_gate, e_up, e_down, rows = inputs
        picked = normed[rows]
        gate = jnp.dot(picked, e_gate, preferred_element_type=jnp.float32)
        up = jnp.dot(picked, e_up, preferred_element_type=jnp.float32)
        hidden = (jax.nn.silu(gate) * up).astype(jnp.bfloat16)
        total = jnp.zeros((picked.shape[0], D), jnp.float32)
        for index in range(N_TP):
            partial_value = jnp.dot(hidden[:, index * block:(index + 1) * block], e_down[index * block:(index + 1) * block], preferred_element_type=jnp.float32).astype(jnp.bfloat16)
            total = total + lax.optimization_barrier(partial_value).astype(jnp.float32)
        return total.astype(jnp.bfloat16)
    outputs = lax.map(run_expert, (gate_w, up_w, down_w, owners))
    weighted = outputs.astype(jnp.float32) * weights[:, :, None]
    mixed = jnp.zeros((tokens.shape[0], D), jnp.float32).at[owners.reshape(-1)].add(weighted.reshape(-1, D))
    return (gate_w, up_w, down_w, mixed.astype(jnp.bfloat16))
```

```python
import jax
import jax.numpy as jnp
from jax import lax
from jax.sharding import Mesh
from jax.sharding import PartitionSpec as P

FS = ("z", "core")
GRP_FS = ("grp", "z", "core")


def after(value, *earlier):
    return lax.optimization_barrier((value, *earlier))[0]


def along_z(pieces):
    return lax.all_to_all(pieces, "z", split_axis=0, concat_axis=0, tiled=True)


def sorted_by_core(pieces):
    core = lax.axis_index("core")
    mine = lax.dynamic_index_in_dim(pieces, core, 1, keepdims=False)
    other = lax.dynamic_index_in_dim(pieces, 1 - core, 1, keepdims=False)
    got = lax.ppermute(other, "core", [(0, 1), (1, 0)])
    first = core == 0
    return jnp.stack([jnp.where(first, mine, got), jnp.where(first, got, mine)], axis=1)


def by_shift(axis, sign, shift):
    count = lax.axis_size(axis)
    return [(i, (i + sign * shift) % count) for i in range(count)]


def shards(tokens, norm_gain, gate_master, up_master, down_master, expert_ids, route_weights):
    bf16, f32 = jnp.bfloat16, jnp.float32
    groups, own_group = lax.axis_size("grp"), lax.axis_index("grp")
    nz, cores = lax.axis_size("z"), lax.axis_size("core")
    n_tp, own_tp = lax.axis_size("tp"), lax.axis_index("tp")
    experts, block_rows, ff_block = gate_master.shape
    count, width = tokens.shape
    top = expert_ids.shape[1]
    capacity = top * count // experts

    share = block_rows // groups

    def shared(master):
        piece = lax.dynamic_slice_in_dim(master, own_group * share, share, 1)
        gain = lax.dynamic_slice_in_dim(norm_gain, own_group * share, share, 0)
        return (gain[None, :, None] * piece).astype(bf16)

    gate_up = jnp.stack([shared(gate_master), shared(up_master)], axis=1)
    gate_up = sorted_by_core(gate_up.reshape(nz, cores, 2, share, ff_block))
    gate_up_z = along_z(gate_up)

    down_rows = down_master.shape[1]
    down_share = down_rows // groups
    down = lax.dynamic_slice_in_dim(down_master, own_group * down_share, down_share, 1).astype(bf16)
    if down_share % 8:
        down = down.reshape(experts, -1, ff_block)
    down = sorted_by_core(down.reshape(nz, cores, *down.shape[1:]))

    values = tokens.astype(f32)
    squares = jnp.sum(values * values, axis=1)
    squares = jnp.sum(lax.all_gather(squares, "tp", axis=0), axis=0)
    normed = (values * lax.rsqrt(squares / (width * n_tp) + 1e-06)[:, None]).astype(bf16)

    ids = expert_ids.T
    names = jnp.arange(experts, dtype=jnp.int32)[:, None]
    hits = [ids[k][None, :] == names for k in range(top)]
    named = sum(h.astype(f32) for h in hits)
    weight = sum(jnp.where(h, route_weights[:, k][None, :], 0.0) for k, h in enumerate(hits))
    earlier = jnp.arange(count)[:, None] < jnp.arange(count)[None, :]
    place = jnp.dot(named.astype(bf16), earlier.astype(bf16), preferred_element_type=f32)
    place = jnp.where(named > 0, place, -1.0).astype(jnp.int32)
    high = lax.reduce_precision(weight, 8, 7)
    low = weight - high

    first = capacity * 2 // 3 // 8 * 8
    chunks = [(0, first), (first, capacity - first)]

    def chosen(start, size):
        at = jnp.arange(size, dtype=jnp.int32)[None, :, None] + start
        return place[:, None, :] == at

    def sent(start, size):
        pick = chosen(start, size).astype(bf16).reshape(experts * size, count)
        rows = jnp.dot(pick, normed, preferred_element_type=f32).astype(bf16)
        return sorted_by_core(rows.reshape(nz, cores, size, width))

    def mixed_of(start, size, rows):
        hit = chosen(start, size)
        rows = rows.reshape(experts * size, width)
        total = 0.0
        for part in (high, low):
            w = jnp.where(hit, part[:, None, :], 0.0).astype(bf16).reshape(experts * size, count)
            total = total + lax.dot_general(w, rows, (((0,), (0,)), ((), ())), preferred_element_type=f32)
        return total

    outbound = [sent(*c) for c in chunks]
    rows_a = along_z(after(outbound[0], gate_up_z))
    down_z = along_z(after(down, rows_a))
    rows_b = along_z(after(outbound[1], down_z))

    whole = lax.all_gather(gate_up_z, "grp", axis=0)
    whole = jnp.moveaxis(whole, 0, 3).reshape(nz, cores, 2, block_rows, ff_block)
    gate_local = whole[:, :, 0].reshape(-1, ff_block)
    up_local = whole[:, :, 1].reshape(-1, ff_block)
    weights = []
    for shift in range(n_tp):
        start = (own_tp - shift) % n_tp * width
        piece = jnp.concatenate(
            [lax.dynamic_slice_in_dim(w, start, width, 0) for w in (gate_local, up_local)], axis=1
        )
        if shift:
            piece = lax.ppermute(piece, "tp", by_shift("tp", -1, shift))
        weights.append(piece)

    down_whole = lax.all_gather(down_z, "grp", axis=0)
    down_whole = down_whole.reshape(groups, nz, cores, down_share, width)
    down_whole = jnp.moveaxis(down_whole, 0, 2).reshape(-1, width)
    down_local = jnp.zeros((ff_block, width * n_tp), bf16)
    for shift in range(n_tp):
        piece = lax.dynamic_slice_in_dim(down_whole, (own_tp - shift) % n_tp * ff_block, ff_block, 0)
        if shift:
            piece = lax.ppermute(piece, "tp", by_shift("tp", -1, shift))
        down_local = lax.dynamic_update_slice_in_dim(
            down_local, piece, (own_tp + shift) % n_tp * width, 1
        )

    def served(rows):
        size = rows.shape[2]
        rows = rows.reshape(-1, width)
        total = None
        for shift in range(1, n_tp):
            part = jnp.dot(rows, weights[shift], preferred_element_type=f32).astype(bf16)
            part = lax.ppermute(part, "tp", by_shift("tp", 1, shift)).astype(f32)
            total = part if total is None else total + part
        total = total + jnp.dot(rows, weights[0], preferred_element_type=f32)
        gate, up = total[:, :ff_block], total[:, ff_block:]
        hidden = (jax.nn.silu(gate) * up).astype(bf16)
        hidden = lax.all_gather(hidden, "tp", axis=1, tiled=True)
        out = jnp.dot(hidden, down_whole, preferred_element_type=f32).astype(bf16)
        return sorted_by_core(out.reshape(nz, cores, size, width))

    back_a = along_z(after(served(rows_a), rows_b))
    back_b = along_z(after(served(rows_b), back_a))
    mixed = mixed_of(*chunks[0], back_a) + mixed_of(*chunks[1], back_b)
    return (gate_local[None], up_local[None], down_local[None], mixed.astype(bf16))


def solution(mesh):
    torus = Mesh(
        mesh.devices.reshape(mesh.shape["grp"], -1, 2, mesh.shape["tp"]),
        ("grp", "z", "core", "tp"),
    )
    return jax.shard_map(
        shards,
        mesh=torus,
        in_specs=(
            P(GRP_FS, "tp"),
            P(FS),
            P(None, FS, "tp"),
            P(None, FS, "tp"),
            P(None, FS, "tp"),
            P(GRP_FS, None),
            P(GRP_FS, None),
        ),
        out_specs=(
            P(GRP_FS, None, "tp"),
            P(GRP_FS, None, "tp"),
            P(GRP_FS, "tp", None),
            P(GRP_FS, "tp"),
        ),
        check_vma=False,
    )
```

```python
import jax
import jax.numpy as jnp
from jax import lax
from jax.sharding import Mesh
from jax.sharding import PartitionSpec as P

FS = ("z", "core")
GRP_FS = ("grp", "z", "core")
MEMBERS = 8


def after(value, *earlier):
    return lax.optimization_barrier((value, *earlier))[0]


def along_z(pieces):
    return lax.all_to_all(pieces, "z", split_axis=0, concat_axis=0, tiled=True)


def sorted_by_core(pieces):
    core = lax.axis_index("core")
    mine = lax.dynamic_index_in_dim(pieces, core, 1, keepdims=False)
    other = lax.dynamic_index_in_dim(pieces, 1 - core, 1, keepdims=False)
    got = lax.ppermute(other, "core", [(0, 1), (1, 0)])
    first = core == 0
    return jnp.stack([jnp.where(first, mine, got), jnp.where(first, got, mine)], axis=1)


def by_shift(axis, sign, shift):
    count = lax.axis_size(axis)
    return [(i, (i + sign * shift) % count) for i in range(count)]


def routes_of(count, members):
    parts = count // members

    def route(toward, across):
        pairs = []
        for i in range(count):
            part, at = i // members, i % members
            lower = at < members // 2
            part += {"away": 1 if lower else -1, "back": -1 if lower else 1, "far": 2}[toward]
            pairs.append((i, part % parts * members + (at ^ (members // 2) if across else at)))
        return pairs

    return route("away", False), route("back", True), route("far", True)


def shards(tokens, norm_gain, gate_master, up_master, down_master, expert_ids, route_weights):
    bf16, f32 = jnp.bfloat16, jnp.float32
    groups, own_group = lax.axis_size("grp"), lax.axis_index("grp")
    nz, cores = lax.axis_size("z"), lax.axis_size("core")
    n_tp, own_tp = lax.axis_size("tp"), lax.axis_index("tp")
    experts, block_rows, ff_block = gate_master.shape
    count, width = tokens.shape
    top = expert_ids.shape[1]
    capacity = top * count // experts

    share = block_rows // groups

    def shared(master):
        piece = lax.dynamic_slice_in_dim(master, own_group * share, share, 1)
        gain = lax.dynamic_slice_in_dim(norm_gain, own_group * share, share, 0)
        return (gain[None, :, None] * piece).astype(bf16)

    gate_up = jnp.stack([shared(gate_master), shared(up_master)], axis=1)
    gate_up = sorted_by_core(gate_up.reshape(nz, cores, 2, share, ff_block))
    gate_up_z = along_z(gate_up)

    down_rows = down_master.shape[1]
    down_share = down_rows // groups
    down = lax.dynamic_slice_in_dim(down_master, own_group * down_share, down_share, 1).astype(bf16)
    if down_share % 8:
        down = down.reshape(experts, -1, ff_block)
    down = sorted_by_core(down.reshape(nz, cores, *down.shape[1:]))

    served_by = lax.axis_size(FS) // (experts // MEMBERS)
    own = lax.axis_index(FS)
    own_part, own_place = own // served_by, own % served_by
    parts = experts // MEMBERS
    step = jnp.where(own_place < served_by // 2, 1, -1)
    targets = [own_part, (own_part + step) % parts, (own_part - step) % parts, (own_part + 2) % parts]
    routes = [None, *routes_of(lax.axis_size(FS), served_by)]

    ids = expert_ids.T
    names = jnp.arange(experts, dtype=jnp.int32)[:, None]
    hits = [ids[k][None, :] == names for k in range(top)]
    named = sum(h.astype(f32) for h in hits)
    weight = sum(jnp.where(h, route_weights[:, k][None, :], 0.0) for k, h in enumerate(hits))
    part_of = (ids[0] // MEMBERS)[None, :]
    in_part = jnp.concatenate([(part_of == t).astype(f32) for t in targets], axis=0)
    earlier = jnp.arange(count)[:, None] < jnp.arange(count)[None, :]
    before = jnp.dot(
        jnp.concatenate([named, in_part], axis=0).astype(bf16),
        earlier.astype(bf16),
        preferred_element_type=f32,
    )
    place = jnp.where(named > 0, before[:experts], -1.0)
    rank = jnp.where(in_part > 0, before[experts:], -1.0).astype(jnp.int32)
    high = lax.reduce_precision(weight, 8, 7)
    low = weight - high
    table = jnp.stack([place, high, low]).astype(bf16)

    block = count // parts
    slot = jnp.arange(block, dtype=jnp.int32)[None, :, None]
    order = (rank[:, None, :] == slot).astype(bf16)
    notes = []
    for k, target in enumerate(targets):
        note = lax.dynamic_slice_in_dim(table, target * MEMBERS, MEMBERS, 1)
        note = lax.dot_general(
            note.reshape(-1, count), order[k], (((1,), (1,)), ((), ())), preferred_element_type=f32
        ).astype(bf16)
        notes.append(lax.ppermute(note, FS, routes[k]) if k else note)

    values = tokens.astype(f32)
    squares = jnp.sum(values * values, axis=1)
    squares = jnp.sum(lax.all_gather(squares, "tp", axis=0), axis=0)
    normed = (values * lax.rsqrt(squares / (width * n_tp) + 1e-06)[:, None]).astype(bf16)

    normed = after(normed, gate_up_z)
    landed = []
    for k in range(len(targets)):
        rows = jnp.dot(order[k], normed, preferred_element_type=f32).astype(bf16)
        landed.append(lax.ppermute(rows, FS, routes[k]) if k else rows)

    down_z = along_z(after(down, gate_up_z))

    def by_partner(values):
        rest = values.shape[1:]
        values = values.reshape(2, 2, 2, *rest)
        for bit in range(3):
            flip = (own_place >> (2 - bit)) & 1 == 1
            values = jnp.where(flip, jnp.flip(values, bit), values)
        return values.reshape(-1, *rest)

    def to_partners(pieces):
        return [
            lax.ppermute(p, FS, [(i, i ^ k) for i in range(lax.axis_size(FS))]) if k else p
            for k, p in enumerate(pieces)
        ]

    per_partner = 2 * capacity

    def chosen(blocks):
        note = jnp.concatenate([notes[k] for k in blocks], axis=1).astype(f32)
        note = note.reshape(3, MEMBERS, -1)
        offset = jnp.arange(note.shape[2], dtype=jnp.int32)[None, :] // block * capacity
        places = by_partner(note[0]).astype(jnp.int32)
        places = jnp.where(places >= 0, places + offset, -1)
        at = jnp.arange(per_partner, dtype=jnp.int32)[None, :, None]
        hit = places[:, None, :] == at
        return hit, by_partner(note[1]), by_partner(note[2])

    def sent(blocks, hit):
        rows = jnp.concatenate([landed[k] for k in blocks], axis=0)
        pick = hit.astype(bf16)
        rows = [
            jnp.dot(pick[k], rows, preferred_element_type=f32).astype(bf16) for k in range(MEMBERS)
        ]
        return jnp.concatenate(to_partners(rows), axis=0)

    def mixed_of(out, hit, *scales):
        back = to_partners([out[k * per_partner : (k + 1) * per_partner] for k in range(MEMBERS)])
        back = jnp.concatenate(back, axis=0)
        total = 0.0
        for scale in scales:
            w = jnp.where(hit, scale[:, None, :], 0.0).astype(bf16).reshape(back.shape[0], -1)
            total = total + lax.dot_general(w, back, (((0,), (0,)), ((), ())), preferred_element_type=f32)
        return total.astype(bf16)

    whole = lax.all_gather(gate_up_z, "grp", axis=0)
    whole = jnp.moveaxis(whole, 0, 3).reshape(nz, cores, 2, block_rows, ff_block)
    gate_local = whole[:, :, 0].reshape(-1, ff_block)
    up_local = whole[:, :, 1].reshape(-1, ff_block)
    weights = []
    for shift in range(n_tp):
        start = (own_tp - shift) % n_tp * width
        piece = jnp.concatenate(
            [lax.dynamic_slice_in_dim(w, start, width, 0) for w in (gate_local, up_local)], axis=1
        )
        if shift:
            piece = lax.ppermute(piece, "tp", by_shift("tp", -1, shift))
        weights.append(piece)

    down_whole = lax.all_gather(down_z, "grp", axis=0)
    down_whole = down_whole.reshape(groups, nz, cores, down_share, width)
    down_whole = jnp.moveaxis(down_whole, 0, 2).reshape(-1, width)
    down_local = jnp.zeros((ff_block, width * n_tp), bf16)
    for shift in range(n_tp):
        piece = lax.dynamic_slice_in_dim(down_whole, (own_tp - shift) % n_tp * ff_block, ff_block, 0)
        if shift:
            piece = lax.ppermute(piece, "tp", by_shift("tp", -1, shift))
        down_local = lax.dynamic_update_slice_in_dim(
            down_local, piece, (own_tp + shift) % n_tp * width, 1
        )

    def served(rows):
        total = None
        for shift in range(1, n_tp):
            part = jnp.dot(rows, weights[shift], preferred_element_type=f32).astype(bf16)
            part = lax.ppermute(part, "tp", by_shift("tp", 1, shift)).astype(f32)
            total = part if total is None else total + part
        total = total + jnp.dot(rows, weights[0], preferred_element_type=f32)
        gate, up = total[:, :ff_block], total[:, ff_block:]
        hidden = (jax.nn.silu(gate) * up).astype(bf16)
        hidden = lax.all_gather(hidden, "tp", axis=1, tiled=True)
        return jnp.dot(hidden, down_whole, preferred_element_type=f32).astype(bf16)

    chunks = [(0, 2), (1, 3)]
    picks = [chosen(c) for c in chunks]
    rows = [sent(c, pick[0]) for c, pick in zip(chunks, picks)]
    home = [None] * len(targets)
    for c, pick, piece in zip(chunks, picks, rows):
        done = mixed_of(served(piece), *pick)
        for n, k in enumerate(c):
            part = done[n * block : (n + 1) * block]
            home[k] = lax.ppermute(part, FS, [(b, a) for a, b in routes[k]]) if k else part
    mixed = lax.dot_general(
        order.reshape(count, count),
        jnp.concatenate(home, axis=0),
        (((0,), (0,)), ((), ())),
        preferred_element_type=f32,
    ).astype(bf16)
    return (gate_local[None], up_local[None], down_local[None], mixed)


def solution(mesh):
    torus = Mesh(
        mesh.devices.reshape(mesh.shape["grp"], -1, 2, mesh.shape["tp"]),
        ("grp", "z", "core", "tp"),
    )
    return jax.shard_map(
        shards,
        mesh=torus,
        in_specs=(
            P(GRP_FS, "tp"),
            P(FS),
            P(None, FS, "tp"),
            P(None, FS, "tp"),
            P(None, FS, "tp"),
            P(GRP_FS, None),
            P(GRP_FS, None),
        ),
        out_specs=(
            P(GRP_FS, None, "tp"),
            P(GRP_FS, None, "tp"),
            P(GRP_FS, "tp", None),
            P(GRP_FS, "tp"),
        ),
        check_vma=False,
    )
```

```python
import jax
import jax.numpy as jnp
from jax import lax
from jax.sharding import Mesh
from jax.sharding import PartitionSpec as P

FS = ("z", "core")
GRP_FS = ("grp", "z", "core")


def after(value, *earlier):
    return lax.optimization_barrier((value, *earlier))[0]


def along_z(pieces):
    return lax.all_to_all(pieces, "z", split_axis=0, concat_axis=0, tiled=True)


def sorted_by_core(pieces):
    core = lax.axis_index("core")
    mine = lax.dynamic_index_in_dim(pieces, core, 1, keepdims=False)
    other = lax.dynamic_index_in_dim(pieces, 1 - core, 1, keepdims=False)
    got = lax.ppermute(other, "core", [(0, 1), (1, 0)])
    first = core == 0
    return jnp.stack([jnp.where(first, mine, got), jnp.where(first, got, mine)], axis=1)


def by_shift(axis, sign, shift):
    count = lax.axis_size(axis)
    return [(i, (i + sign * shift) % count) for i in range(count)]


def shards(tokens, norm_gain, gate_master, up_master, down_master, expert_ids, route_weights):
    bf16, f32 = jnp.bfloat16, jnp.float32
    groups, own_group = lax.axis_size("grp"), lax.axis_index("grp")
    nz, cores = lax.axis_size("z"), lax.axis_size("core")
    n_tp, own_tp = lax.axis_size("tp"), lax.axis_index("tp")
    experts, block_rows, ff_block = gate_master.shape
    count, width = tokens.shape
    top = expert_ids.shape[1]
    capacity = top * count // experts

    share = block_rows // groups

    def shared(master):
        piece = lax.dynamic_slice_in_dim(master, own_group * share, share, 1)
        gain = lax.dynamic_slice_in_dim(norm_gain, own_group * share, share, 0)
        return (gain[None, :, None] * piece).astype(bf16)

    down_rows = down_master.shape[1]
    down_share = down_rows // groups
    down = lax.dynamic_slice_in_dim(down_master, own_group * down_share, down_share, 1).astype(bf16)
    down = down.reshape(experts, -1, ff_block)
    sent_rows = jnp.concatenate([shared(gate_master), shared(up_master), down], axis=1)
    sent_rows = sorted_by_core(sent_rows.reshape(nz, cores, -1, ff_block))
    weights_z = along_z(sent_rows)
    gate_up_z = weights_z[:, :, : 2 * share].reshape(nz, cores, 2, share, ff_block)
    down_z = weights_z[:, :, 2 * share :]

    values = tokens.astype(f32)
    squares = jnp.sum(values * values, axis=1)
    squares = jnp.sum(lax.all_gather(squares, "tp", axis=0), axis=0)
    normed = (values * lax.rsqrt(squares / (width * n_tp) + 1e-06)[:, None]).astype(bf16)

    ids = expert_ids.T
    names = jnp.arange(experts, dtype=jnp.int32)[:, None]
    hits = [ids[k][None, :] == names for k in range(top)]
    named = sum(h.astype(f32) for h in hits)
    weight = sum(jnp.where(h, route_weights[:, k][None, :], 0.0) for k, h in enumerate(hits))
    earlier = jnp.arange(count)[:, None] < jnp.arange(count)[None, :]
    place = jnp.dot(named.astype(bf16), earlier.astype(bf16), preferred_element_type=f32)
    place = jnp.where(named > 0, place, -1.0).astype(jnp.int32)
    high = lax.reduce_precision(weight, 8, 7)
    low = weight - high

    first = capacity // 3 // 8 * 8
    chunks = [(0, first), (first, capacity - first)]

    def chosen(start, size):
        at = jnp.arange(size, dtype=jnp.int32)[None, :, None] + start
        return place[:, None, :] == at

    def sent(start, size):
        pick = chosen(start, size).astype(bf16).reshape(experts * size, count)
        rows = jnp.dot(pick, normed, preferred_element_type=f32).astype(bf16)
        return sorted_by_core(rows.reshape(nz, cores, size, width))

    def mixed_of(start, size, rows):
        hit = chosen(start, size)
        rows = rows.reshape(experts * size, width)
        total = 0.0
        for part in (high, low):
            w = jnp.where(hit, part[:, None, :], 0.0).astype(bf16).reshape(experts * size, count)
            total = total + lax.dot_general(w, rows, (((0,), (0,)), ((), ())), preferred_element_type=f32)
        return total

    outbound = [sent(*c) for c in chunks]
    rows_a = along_z(after(outbound[0], weights_z))
    rows_b = along_z(after(outbound[1], rows_a))

    whole = lax.all_gather(gate_up_z, "grp", axis=0)
    whole = jnp.moveaxis(whole, 0, 3).reshape(nz, cores, 2, block_rows, ff_block)
    gate_local = whole[:, :, 0].reshape(-1, ff_block)
    up_local = whole[:, :, 1].reshape(-1, ff_block)
    weights = []
    for shift in range(n_tp):
        start = (own_tp - shift) % n_tp * width
        piece = jnp.concatenate(
            [lax.dynamic_slice_in_dim(w, start, width, 0) for w in (gate_local, up_local)], axis=1
        )
        if shift:
            piece = lax.ppermute(piece, "tp", by_shift("tp", -1, shift))
        weights.append(piece)

    def products(rows):
        first, *others = [jnp.dot(rows, w, preferred_element_type=f32) for w in weights]
        return [first, *(p.astype(bf16) for p in others)]

    products_a = products(rows_a.reshape(-1, width))

    down_whole = after(lax.all_gather(after(down_z, whole), "grp", axis=0), *products_a[1:])
    down_whole = down_whole.reshape(groups, nz, cores, down_share, width)
    down_whole = jnp.moveaxis(down_whole, 0, 2).reshape(-1, width)
    down_parts = [
        lax.dynamic_slice_in_dim(down_whole, (own_tp + shift) % n_tp * ff_block, ff_block, 0)
        for shift in range(n_tp)
    ]
    down_local = jnp.zeros((ff_block, width * n_tp), bf16)
    for shift in range(n_tp):
        piece = lax.dynamic_slice_in_dim(down_whole, (own_tp - shift) % n_tp * ff_block, ff_block, 0)
        if shift:
            piece = lax.ppermute(piece, "tp", by_shift("tp", -1, shift))
        down_local = lax.dynamic_update_slice_in_dim(
            down_local, piece, (own_tp + shift) % n_tp * width, 1
        )

    def served(products, size):
        total = products[0]
        for shift in range(1, n_tp):
            part = lax.ppermute(products[shift], "tp", by_shift("tp", 1, shift))
            total = total + part.astype(f32)
        gate, up = total[:, :ff_block], total[:, ff_block:]
        hidden = (jax.nn.silu(gate) * up).astype(bf16)
        out = jnp.dot(hidden, down_parts[0], preferred_element_type=f32)
        for shift in range(1, n_tp):
            piece = lax.ppermute(hidden, "tp", by_shift("tp", -1, shift))
            out = out + jnp.dot(piece, down_parts[shift], preferred_element_type=f32)
        out = out.astype(bf16)
        return out.reshape(nz, cores, size, width)

    back_a = along_z(after(served(products_a, chunks[0][1]), rows_b))
    products_b = products(rows_b.reshape(-1, width))
    back_b = along_z(after(sorted_by_core(served(products_b, chunks[1][1])), back_a))
    mixed = mixed_of(*chunks[0], sorted_by_core(back_a)) + mixed_of(*chunks[1], back_b)
    return (gate_local[None], up_local[None], down_local[None], mixed.astype(bf16))


def solution(mesh):
    torus = Mesh(
        mesh.devices.reshape(mesh.shape["grp"], -1, 2, mesh.shape["tp"]),
        ("grp", "z", "core", "tp"),
    )
    return jax.shard_map(
        shards,
        mesh=torus,
        in_specs=(
            P(GRP_FS, "tp"),
            P(FS),
            P(None, FS, "tp"),
            P(None, FS, "tp"),
            P(None, FS, "tp"),
            P(GRP_FS, None),
            P(GRP_FS, None),
        ),
        out_specs=(
            P(GRP_FS, None, "tp"),
            P(GRP_FS, None, "tp"),
            P(GRP_FS, "tp", None),
            P(GRP_FS, "tp"),
        ),
        check_vma=False,
    )
```

```python
import jax
import jax.numpy as jnp
from jax import lax
from jax.sharding import Mesh
from jax.sharding import PartitionSpec as P

FS = ("z", "core")
GRP_FS = ("grp", "z", "core")


def after(value, *earlier):
    return lax.optimization_barrier((value, *earlier))[0]


def along_z(pieces):
    return lax.all_to_all(pieces, "z", split_axis=0, concat_axis=0, tiled=True)


def sorted_by_core(pieces):
    core = lax.axis_index("core")
    mine = lax.dynamic_index_in_dim(pieces, core, 1, keepdims=False)
    other = lax.dynamic_index_in_dim(pieces, 1 - core, 1, keepdims=False)
    got = lax.ppermute(other, "core", [(0, 1), (1, 0)])
    first = core == 0
    return jnp.stack([jnp.where(first, mine, got), jnp.where(first, got, mine)], axis=1)


def by_shift(axis, sign, shift):
    count = lax.axis_size(axis)
    return [(i, (i + sign * shift) % count) for i in range(count)]


def shards(tokens, norm_gain, gate_master, up_master, down_master, expert_ids, route_weights):
    bf16, f32 = jnp.bfloat16, jnp.float32
    groups, own_group = lax.axis_size("grp"), lax.axis_index("grp")
    nz, cores = lax.axis_size("z"), lax.axis_size("core")
    n_tp, own_tp = lax.axis_size("tp"), lax.axis_index("tp")
    experts, block_rows, ff_block = gate_master.shape
    count, width = tokens.shape
    top = expert_ids.shape[1]
    capacity = top * count // experts

    share = block_rows // groups

    def shared(master):
        piece = lax.dynamic_slice_in_dim(master, own_group * share, share, 1)
        gain = lax.dynamic_slice_in_dim(norm_gain, own_group * share, share, 0)
        return (gain[None, :, None] * piece).astype(bf16)

    down_rows = down_master.shape[1]
    down_share = down_rows // groups
    down = lax.dynamic_slice_in_dim(down_master, own_group * down_share, down_share, 1).astype(bf16)
    down = down.reshape(experts, -1, ff_block)
    sent_rows = jnp.concatenate([shared(gate_master), shared(up_master), down], axis=1)
    sent_rows = sorted_by_core(sent_rows.reshape(nz, cores, -1, ff_block))
    weights_z = along_z(sent_rows)
    gate_up_z = weights_z[:, :, : 2 * share].reshape(nz, cores, 2, share, ff_block)
    down_z = weights_z[:, :, 2 * share :]

    values = tokens.astype(f32)
    squares = jnp.sum(values * values, axis=1)
    squares = jnp.sum(lax.all_gather(squares, "tp", axis=0), axis=0)
    normed = (values * lax.rsqrt(squares / (width * n_tp) + 1e-06)[:, None]).astype(bf16)

    ids = expert_ids.T
    names = jnp.arange(experts, dtype=jnp.int32)[:, None]
    hits = [ids[k][None, :] == names for k in range(top)]
    named = sum(h.astype(f32) for h in hits)
    weight = sum(jnp.where(h, route_weights[:, k][None, :], 0.0) for k, h in enumerate(hits))
    earlier = jnp.arange(count)[:, None] < jnp.arange(count)[None, :]
    place = jnp.dot(named.astype(bf16), earlier.astype(bf16), preferred_element_type=f32)
    place = jnp.where(named > 0, place, -1.0).astype(jnp.int32)
    high = lax.reduce_precision(weight, 8, 7)
    low = weight - high

    first = capacity // 3 // 8 * 8
    chunks = [(0, first), (first, capacity - first)]

    def chosen(start, size):
        at = jnp.arange(size, dtype=jnp.int32)[None, :, None] + start
        return place[:, None, :] == at

    def sent(start, size):
        pick = chosen(start, size).astype(bf16).reshape(experts * size, count)
        rows = jnp.dot(pick, normed, preferred_element_type=f32).astype(bf16)
        return sorted_by_core(rows.reshape(nz, cores, size, width))

    def mixed_of(start, size, rows, tables):
        places, *scales = tables
        at = jnp.arange(size, dtype=jnp.int32)[None, :, None] + start
        hit = places[:, None, :] == at
        rows = rows.reshape(-1, width)
        total = 0.0
        for part in scales:
            w = jnp.where(hit, part[:, None, :], 0.0).astype(bf16).reshape(-1, count)
            total = total + lax.dot_general(w, rows, (((0,), (0,)), ((), ())), preferred_element_type=f32)
        return total

    def of_core(values, core):
        return lax.dynamic_index_in_dim(values.reshape(nz, cores, count), core, 1, keepdims=False)

    outbound = [sent(*c) for c in chunks]
    rows_a = along_z(after(outbound[0], weights_z))
    rows_b = along_z(after(outbound[1], rows_a))

    whole = lax.all_gather(gate_up_z, "grp", axis=0)
    whole = jnp.moveaxis(whole, 0, 3).reshape(nz, cores, 2, block_rows, ff_block)
    gate_local = whole[:, :, 0].reshape(-1, ff_block)
    up_local = whole[:, :, 1].reshape(-1, ff_block)
    weights = []
    for shift in range(n_tp):
        start = (own_tp - shift) % n_tp * width
        piece = jnp.concatenate(
            [lax.dynamic_slice_in_dim(w, start, width, 0) for w in (gate_local, up_local)], axis=1
        )
        if shift:
            piece = lax.ppermute(piece, "tp", by_shift("tp", -1, shift))
        weights.append(piece)

    def products(rows):
        first, *others = [jnp.dot(rows, w, preferred_element_type=f32) for w in weights]
        return [first, *(p.astype(bf16) for p in others)]

    products_a = products(rows_a.reshape(-1, width))

    down_whole = after(lax.all_gather(after(down_z, whole), "grp", axis=0), *products_a[1:])
    down_whole = down_whole.reshape(groups, nz, cores, down_share, width)
    down_whole = jnp.moveaxis(down_whole, 0, 2).reshape(-1, width)
    down_parts = [
        lax.dynamic_slice_in_dim(down_whole, (own_tp + shift) % n_tp * ff_block, ff_block, 0)
        for shift in range(n_tp)
    ]
    down_local = jnp.zeros((ff_block, width * n_tp), bf16)
    for shift in range(n_tp):
        piece = lax.dynamic_slice_in_dim(down_whole, (own_tp - shift) % n_tp * ff_block, ff_block, 0)
        if shift:
            piece = lax.ppermute(piece, "tp", by_shift("tp", -1, shift))
        down_local = lax.dynamic_update_slice_in_dim(
            down_local, piece, (own_tp + shift) % n_tp * width, 1
        )

    def served(products, size):
        total = products[0]
        for shift in range(1, n_tp):
            part = lax.ppermute(products[shift], "tp", by_shift("tp", 1, shift))
            total = total + part.astype(f32)
        gate, up = total[:, :ff_block], total[:, ff_block:]
        hidden = (jax.nn.silu(gate) * up).astype(bf16)
        out = jnp.dot(hidden, down_parts[0], preferred_element_type=f32)
        for shift in range(1, n_tp):
            piece = lax.ppermute(hidden, "tp", by_shift("tp", -1, shift))
            out = out + jnp.dot(piece, down_parts[shift], preferred_element_type=f32)
        out = out.astype(bf16)
        return out.reshape(nz, cores, size, width)

    back_a = along_z(after(served(products_a, chunks[0][1]), rows_b))
    products_b = products(rows_b.reshape(-1, width))
    back_b = along_z(after(served(products_b, chunks[1][1]), back_a))
    core = lax.axis_index("core")
    own, sibling = [
        lax.dynamic_index_in_dim(back_b, c, 1, keepdims=False) for c in (core, 1 - core)
    ]
    sibling = lax.ppermute(sibling, "core", [(0, 1), (1, 0)])
    tables = (place, high, low)
    mixed = mixed_of(*chunks[0], sorted_by_core(back_a), tables)
    for c, rows in ((core, own), (1 - core, sibling)):
        mixed = mixed + mixed_of(*chunks[1], rows, [of_core(v, c) for v in tables])
    return (gate_local[None], up_local[None], down_local[None], mixed.astype(bf16))


def solution(mesh):
    torus = Mesh(
        mesh.devices.reshape(mesh.shape["grp"], -1, 2, mesh.shape["tp"]),
        ("grp", "z", "core", "tp"),
    )
    return jax.shard_map(
        shards,
        mesh=torus,
        in_specs=(
            P(GRP_FS, "tp"),
            P(FS),
            P(None, FS, "tp"),
            P(None, FS, "tp"),
            P(None, FS, "tp"),
            P(GRP_FS, None),
            P(GRP_FS, None),
        ),
        out_specs=(
            P(GRP_FS, None, "tp"),
            P(GRP_FS, None, "tp"),
            P(GRP_FS, "tp", None),
            P(GRP_FS, "tp"),
        ),
        check_vma=False,
    )
```
